32 devices in a mesh: fs: 4 (over z), rep: 4 (over y, x), tp: 2 (over core).
Axes of the slice: x: 2, y: 2, z: 4, core: 2. Of those that a mesh axis runs over, the one named last changes fastest.
Arguments:
- saved_inputs: bfloat16 [12288, 2048], P(('fs', 'rep')), may hold values from -6 to 6
- query_cotangent: bfloat16 [12288, 1024], P(('fs', 'rep'), 'tp'), may hold values from -0.053955078 to 0.053955078
- value_cotangent: bfloat16 [12288, 2048], P(('fs', 'rep'), 'tp'), may hold values from -0.053955078 to 0.053955078
- query_weight: float32 [2048, 1024], P('fs', 'tp'), may hold values from -0.125 to 0.125
- value_weight: float32 [2048, 2048], P('fs', 'tp'), may hold values from -0.125 to 0.125
- query_factor: bfloat16 [2048, 256], P('fs'), as said below
- value_factor: bfloat16 [2048, 256], P('fs'), as said below
- query_first: float32 [256, 1024], P('rep', 'tp'), may hold values from -6 to 6
- query_second: float32 [256, 1024], P('rep', 'tp'), may hold values from 0.3 to 3
- value_first: float32 [256, 2048], P('rep', 'tp'), may hold values from -6 to 6
- value_second: float32 [256, 2048], P('rep', 'tp'), may hold values from 0.3 to 3
Outputs:
- query_direction: float32 [2048, 1024], P('fs', 'tp')
- value_direction: float32 [2048, 2048], P('fs', 'tp')
- query_master: float32 [2048, 1024], P('fs', 'tp')
- value_master: float32 [2048, 2048], P('fs', 'tp')
- query_first_new: float32 [256, 1024], P('rep', 'tp')
- query_second_new: float32 [256, 1024], P('rep', 'tp')
- value_first_new: float32 [256, 2048], P('rep', 'tp')
- value_second_new: float32 [256, 2048], P('rep', 'tp')
- query_copy: bfloat16 [2048, 1024], P(None, 'tp')
- value_copy: bfloat16 [2048, 2048], P(None, 'tp')
The draws below stay inside these ranges and needn't reach their ends.
Inputs may be any that keep to these rules, and one draw needn't show every extreme that they name: `query_factor`: A matrix of full rank. `value_factor`: A matrix of full rank.
All inputs are finite; a program needn't handle non-finite values.
Results may differ from the reference program's by a relative error of at most 0.012.
Values may be sent and summed in bfloat16 or wider, within the bound.
A program may use at most 128 MiB of HBM per device.

```python
import math
import jax
import jax.numpy as jnp
from jax import lax

D = 2048
QK = 1024
VW = 2048
RANK = 256
TOKENS = 12288


def factor_draw(key):
    first_key, second_key = jax.random.split(key)
    positions = jnp.arange(D, dtype=jnp.float32)
    trend = jnp.exp(math.log(3.0) * positions / D)
    spread = jnp.exp(jax.random.uniform(first_key, (D, 1), jnp.float32, 0.0, math.log(10.0)))
    base = jax.random.normal(second_key, (D, RANK), jnp.float32)
    return (base * spread * trend[:, None] * (0.3 / math.sqrt(D))).astype(jnp.bfloat16)


def draw_query_factor(key, part):
    return factor_draw(jax.random.fold_in(key, 11))


def draw_value_factor(key, part):
    return factor_draw(jax.random.fold_in(key, 23))


def block_levels(stream_key, extent, pieces, least, top_value):
    def one(dim, parts):
        heights = jax.random.uniform(jax.random.fold_in(jax.random.fold_in(stream_key, 6), dim), (parts,), jnp.float32, least / len(pieces), top_value / len(pieces))
        return jnp.repeat(jnp.exp(heights), extent[dim] // parts).reshape((-1,) + (1,) * (len(extent) - dim - 1))

    factor_of = one(*pieces[0])
    for cut in pieces[1:]:
        factor_of = factor_of * one(*cut)
    return factor_of


def normal_values(key, extent, scale, bound, pieces=(), held_as=jnp.bfloat16):
    array = scale * jax.random.normal(key, extent, jnp.float32)
    if pieces:
        array = array * block_levels(key, extent, pieces, -0.22, 0.18)
    return jnp.clip(array, -bound, bound).astype(held_as)


def setup_inputs(seed: int = 0) -> dict:
    keys = jax.random.split(jax.random.key(seed), 12)
    return {
        "saved_inputs": normal_values(keys[0], (TOKENS, D), 1.0, 6.0, ((0, 16),)),
        "query_cotangent": normal_values(keys[1], (TOKENS, QK), (TOKENS ** -0.5), 0.053955078, ((0, 16), (1, 2))),
        "value_cotangent": normal_values(keys[2], (TOKENS, VW), (TOKENS ** -0.5), 0.053955078, ((0, 16), (1, 2))),
        "query_weight": normal_values(keys[3], (D, QK), D ** -0.5, 0.125, ((0, 4), (1, 2)), jnp.float32),
        "value_weight": normal_values(keys[4], (D, VW), D ** -0.5, 0.125, ((0, 4), (1, 2)), jnp.float32),
        "query_factor": draw_query_factor(jax.random.fold_in(keys[11], 71), 0),
        "value_factor": draw_value_factor(jax.random.fold_in(keys[11], 71), 0),
        "query_first": normal_values(keys[7], (RANK, QK), 1.0, 6.0, ((0, 4), (1, 2)), jnp.float32),
        "query_second": jnp.clip(jnp.exp(math.log(3.0) - 2.3025851 * jax.random.uniform(keys[8], (RANK, QK), jnp.float32) ** block_levels(keys[8], (RANK, QK), ((0, 4), (1, 2)), -0.2, 0.2)), 0.3, 3.0),
        "value_first": normal_values(keys[9], (RANK, VW), 1.0, 6.0, ((0, 4), (1, 2)), jnp.float32),
        "value_second": jnp.clip(jnp.exp(math.log(3.0) - 2.3025851 * jax.random.uniform(keys[10], (RANK, VW), jnp.float32) ** block_levels(keys[10], (RANK, VW), ((0, 4), (1, 2)), -0.2, 0.2)), 0.3, 3.0),
    }


BETA_ONE = 0.8
BETA_TWO = 0.9
EPS_RATIO = 1e-08
EPS_NORM = 1e-06
RATE = 0.02

def update_one(grad, factor, weight, first, second):
    wide = factor.astype(jnp.float32)
    projected = jnp.dot(wide.T, grad, precision=lax.Precision.HIGHEST)
    first_new = BETA_ONE * first + (1.0 - BETA_ONE) * projected
    second_new = BETA_TWO * second + (1.0 - BETA_TWO) * projected * projected
    ratio = first_new / (jnp.sqrt(second_new) + EPS_RATIO)
    raw_step = jnp.dot(wide, ratio, precision=lax.Precision.HIGHEST)
    direction = raw_step * lax.rsqrt(jnp.mean(raw_step * raw_step) + EPS_NORM)
    master = weight - RATE * direction
    return (direction, master, first_new, second_new, master.astype(jnp.bfloat16))

def reference(saved_inputs, query_cotangent, value_cotangent, query_weight, value_weight, query_factor, value_factor, query_first, query_second, value_first, value_second):
    dims = (((0,), (0,)), ((), ()))
    query_grad = lax.dot_general(saved_inputs, query_cotangent, dims, preferred_element_type=jnp.float32)
    value_grad = lax.dot_general(saved_inputs, value_cotangent, dims, preferred_element_type=jnp.float32)
    q_dir, q_master, q_first, q_second, q_copy = update_one(query_grad, query_factor, query_weight, query_first, query_second)
    v_dir, v_master, v_first, v_second, v_copy = update_one(value_grad, value_factor, value_weight, value_first, value_second)
    return (q_dir, v_dir, q_master, v_master, q_first, q_second, v_first, v_second, q_copy, v_copy)
```

```python
import jax
import jax.numpy as jnp
from jax import lax
from jax.sharding import PartitionSpec as P

BETA_ONE = 0.8
BETA_TWO = 0.9
EPS_RATIO = 1e-08
EPS_NORM = 1e-06
RATE = 0.02


def moments(projected, first, second):
    first_new = BETA_ONE * first + (1.0 - BETA_ONE) * projected
    second_new = BETA_TWO * second + (1.0 - BETA_TWO) * projected * projected
    ratio = first_new / (jnp.sqrt(second_new) + EPS_RATIO)
    return (first_new, second_new, ratio)


def local(
    saved_inputs,
    query_cotangent,
    value_cotangent,
    query_weight,
    value_weight,
    query_factor,
    value_factor,
    query_first,
    query_second,
    value_first,
    value_second,
):
    qc = query_cotangent.shape[1]
    rank = query_factor.shape[1]
    rows = query_weight.shape[0]
    tp = lax.axis_size("tp")
    bf = jnp.bfloat16
    f32 = jnp.float32
    dims = (((0,), (0,)), ((), ()))
    factors = lax.all_gather(
        jnp.concatenate([query_factor, value_factor], axis=1), "fs", axis=0, tiled=True
    )
    weights = lax.all_gather(
        jnp.concatenate([query_weight.astype(bf), value_weight.astype(bf)], axis=1),
        "fs",
        axis=0,
        tiled=True,
    )
    low = jnp.dot(saved_inputs, factors, preferred_element_type=f32).astype(bf)
    proj = jnp.concatenate(
        [
            lax.dot_general(low[:, :rank], query_cotangent, dims, preferred_element_type=f32),
            lax.dot_general(low[:, rank:], value_cotangent, dims, preferred_element_type=f32),
        ],
        axis=1,
    )
    proj = lax.psum_scatter(proj.astype(bf), "rep", scatter_dimension=0, tiled=True)
    proj = lax.psum(proj.astype(f32), "fs")
    query_first_new, query_second_new, query_ratio = moments(
        proj[:, :qc], query_first, query_second
    )
    value_first_new, value_second_new, value_ratio = moments(
        proj[:, qc:], value_first, value_second
    )
    ratio = jnp.concatenate([query_ratio.astype(bf), value_ratio.astype(bf)], axis=1)
    ratio = lax.all_gather(ratio, "rep", axis=0, tiled=True)
    query_raw = jnp.dot(factors[:, :rank], ratio[:, :qc], preferred_element_type=f32)
    value_raw = jnp.dot(factors[:, rank:], ratio[:, qc:], preferred_element_type=f32)
    query_total, value_total = lax.psum(
        (jnp.sum(query_raw * query_raw), jnp.sum(value_raw * value_raw)), "tp"
    )
    query_scale = lax.rsqrt(query_total / (query_raw.size * tp) + EPS_NORM)
    value_scale = lax.rsqrt(value_total / (value_raw.size * tp) + EPS_NORM)
    query_copy = (weights[:, :qc].astype(f32) - RATE * (query_raw * query_scale)).astype(bf)
    value_copy = (weights[:, qc:].astype(f32) - RATE * (value_raw * value_scale)).astype(bf)
    start = lax.axis_index("fs") * rows
    query_direction = lax.dynamic_slice_in_dim(query_raw, start, rows, 0) * query_scale
    value_direction = lax.dynamic_slice_in_dim(value_raw, start, rows, 0) * value_scale
    query_master = query_weight - RATE * query_direction
    value_master = value_weight - RATE * value_direction
    return (
        query_direction,
        value_direction,
        query_master,
        value_master,
        query_first_new,
        query_second_new,
        value_first_new,
        value_second_new,
        query_copy,
        value_copy,
    )


def solution(mesh):
    return jax.shard_map(
        local,
        mesh=mesh,
        in_specs=(
            P(("fs", "rep"), None),
            P(("fs", "rep"), "tp"),
            P(("fs", "rep"), "tp"),
            P("fs", "tp"),
            P("fs", "tp"),
            P("fs", None),
            P("fs", None),
            P("rep", "tp"),
            P("rep", "tp"),
            P("rep", "tp"),
            P("rep", "tp"),
        ),
        out_specs=(
            P("fs", "tp"),
            P("fs", "tp"),
            P("fs", "tp"),
            P("fs", "tp"),
            P("rep", "tp"),
            P("rep", "tp"),
            P("rep", "tp"),
            P("rep", "tp"),
            P(None, "tp"),
            P(None, "tp"),
        ),
        check_vma=False,
    )
```

```python
import functools

import jax
import jax.numpy as jnp
from jax import lax
from jax.experimental import pallas as pl
from jax.experimental.pallas import tpu as pltpu
from jax.sharding import PartitionSpec as P

BETA_ONE = 0.8
BETA_TWO = 0.9
EPS_RATIO = 1e-08
EPS_NORM = 1e-06
RATE = 0.02
BF = jnp.bfloat16
F32 = jnp.float32


def moments(projected, first, second):
    first_new = BETA_ONE * first + (1.0 - BETA_ONE) * projected
    second_new = BETA_TWO * second + (1.0 - BETA_TWO) * projected * projected
    ratio = first_new / (jnp.sqrt(second_new) + EPS_RATIO)
    return (first_new, second_new, ratio)


def exchange(
    nz,
    nr,
    x_hbm,
    cq_hbm,
    cv_hbm,
    wq_hbm,
    wv_hbm,
    qf_hbm,
    vf_hbm,
    q1_ref,
    q2_ref,
    v1_ref,
    v2_ref,
    w_out,
    f_ref,
    ratio_ref,
    first_out,
    second_out,
    scale_out,
    x_ref,
    cq_ref,
    cv_ref,
    wf_ref,
    wb_ref,
    low_ref,
    part_ref,
    rs_ref,
    z_ref,
    sq_ref,
    local_sem,
    f1_s,
    f1_r,
    w1_s,
    w1_r,
    f2_s,
    f2_r,
    w2_s,
    w2_r,
    rs_s,
    rs_r,
    zs_s,
    zs_r,
    ag_s,
    ag_r,
    tp_s,
    tp_r,
):
    z = lax.axis_index("fs")
    r = lax.axis_index("rep")
    t = lax.axis_index("tp")
    rows = qf_hbm.shape[0]
    part = rows // nr
    qc = cq_ref.shape[1]
    cols = w_out.shape[1]
    half = cols // 2
    width = w_out.shape[0]
    rank = low_ref.shape[2]
    own = rank // nr
    tokens = x_ref.shape[0]
    z_of = [lax.rem(z + k, nz) for k in range(nz)]
    z_from = [lax.rem(z + nz - k, nz) for k in range(nz)]
    r_of = [lax.rem(r + j, nr) for j in range(nr)]
    side = r + 1 - 2 * lax.rem(r, 2)
    over = lax.rem(r + 2, nr)
    corner = nr - 1 - r
    other = 1 - t

    def remote(src, dst, ss, rs, dev):
        return pltpu.make_async_remote_copy(
            src_ref=src,
            dst_ref=dst,
            send_sem=ss,
            recv_sem=rs,
            device_id=dev,
            device_id_type=pl.DeviceIdType.MESH,
        )

    def slab(zz, rr):
        return pl.ds(pl.multiple_of(zz * rows + rr * part, part), part)

    def fac_copy(src):
        return pltpu.make_async_copy(
            src,
            f_ref.at[t, pl.ds(pl.multiple_of(z * rows, rows), rows)],
            local_sem.at[0],
        )

    @pl.when(t == 0)
    def _():
        fac_copy(qf_hbm).start()

    @pl.when(t == 1)
    def _():
        fac_copy(vf_hbm).start()

    wq_in = pltpu.make_async_copy(wq_hbm, wf_ref.at[:, pl.ds(0, qc)], local_sem.at[1])
    wv_in = pltpu.make_async_copy(wv_hbm, wf_ref.at[:, pl.ds(qc, cols - qc)], local_sem.at[2])
    x_in = pltpu.make_async_copy(x_hbm, x_ref, local_sem.at[3])
    cq_in = pltpu.make_async_copy(cq_hbm, cq_ref, local_sem.at[4])
    cv_in = pltpu.make_async_copy(cv_hbm, cv_ref, local_sem.at[5])
    for c in (wq_in, wv_in, x_in, cq_in, cv_in):
        c.start()

    barrier = pltpu.get_barrier_semaphore()
    peers = [(z_of[k], r, t) for k in range(1, nz)]
    peers += [(z, r_of[j], t) for j in range(1, nr)]
    peers += [(z, r, other)]
    for dev in peers:
        pl.semaphore_signal(
            barrier, inc=1, device_id=dev, device_id_type=pl.DeviceIdType.MESH
        )
    pl.semaphore_wait(barrier, len(peers))

    fac_copy(qf_hbm).wait()
    sends = []
    f1 = []
    for k in range(1, nz):
        here = f_ref.at[t, slab(z, r)]
        c = remote(here, here, f1_s.at[k - 1], f1_r.at[k - 1], (z_of[k], r, t))
        c.start()
        f1.append(c)
    wq_in.wait()
    wv_in.wait()
    wb_ref[...] = wf_ref[...].astype(BF)
    w1 = []
    for k in range(1, nz):
        c = remote(
            wb_ref.at[pl.ds(pl.multiple_of(r * part, part), part)],
            w_out.at[slab(z, r)],
            w1_s.at[k - 1],
            w1_r.at[k - 1],
            (z_of[k], r, t),
        )
        c.start()
        w1.append(c)
    w_own = pltpu.make_async_copy(
        wb_ref, w_out.at[pl.ds(pl.multiple_of(z * rows, rows), rows)], local_sem.at[6]
    )
    w_own.start()

    f2 = []
    for k in range(1, nz):
        f1[k - 1].wait_recv()
        there = f_ref.at[t, slab(z_from[k], r)]
        for j in range(1, nr):
            n = (k - 1) * (nr - 1) + j - 1
            c = remote(there, there, f2_s.at[n], f2_r.at[n], (z, r_of[j], t))
            c.start()
            f2.append(c)
    for c in f2:
        c.wait_recv()
    fx = remote(f_ref.at[t], f_ref.at[t], tp_s.at[0], tp_r.at[0], (z, r, other))
    fx.start()
    x_in.wait()
    tile = tokens // 3

    @pl.loop(0, 3)
    def _(i):
        span = pl.ds(pl.multiple_of(i * tile, tile), tile)
        low_ref[t, span] = jnp.dot(
            x_ref[span, :], f_ref[t], preferred_element_type=F32
        ).astype(BF)

    lx = remote(low_ref.at[t], low_ref.at[t], tp_s.at[1], tp_r.at[1], (z, r, other))
    lx.start()
    cq_in.wait()
    cv_in.wait()
    lx.wait_recv()
    dims = (((0,), (0,)), ((), ()))
    part_ref[:, :qc] = lax.dot_general(
        low_ref[0], cq_ref[...], dims, preferred_element_type=F32
    ).astype(BF)
    part_ref[:, qc:] = lax.dot_general(
        low_ref[1], cv_ref[...], dims, preferred_element_type=F32
    ).astype(BF)

    def low_rows(rr):
        return pl.ds(pl.multiple_of(rr * own, own), own)

    rsc = []
    for j in range(1, nr):
        c = remote(
            part_ref.at[low_rows(r_of[j])],
            rs_ref.at[j - 1],
            rs_s.at[j - 1],
            rs_r.at[j - 1],
            (z, r_of[j], t),
        )
        c.start()
        rsc.append(c)

    w2 = {}

    def spread(k):
        w1[k - 1].wait_recv()
        there = w_out.at[slab(z_from[k], r)]
        for n, dev in ((0, side), (1, over)):
            c = remote(there, there, w2_s.at[k - 1, n], w2_r.at[k - 1, n], (z, dev, t))
            c.start()
            w2[k, n] = c

    def relay(k):
        for n, src, dev, at in ((0, side, over, 0), (1, over, side, half)):
            w2[k, n].wait_recv()
            there = w_out.at[slab(z_from[k], src), pl.ds(at, half)]
            c = remote(
                there, there, w2_s.at[k - 1, 2 + n], w2_r.at[k - 1, 2 + n], (z, dev, t)
            )
            c.start()
            w2[k, 2 + n] = c

    stages = [[], [], []]
    for k in range(1, nz):
        stages[min(k - 1, 2)].append(k)
    for c in rsc:
        c.wait_recv()
    total = part_ref[low_rows(r), :].astype(F32)
    for j in range(1, nr):
        total = total + rs_ref[j - 1].astype(F32)
    z_ref[z] = total.astype(BF)
    zc = []
    for k in range(1, nz):
        c = remote(z_ref.at[z], z_ref.at[z], zs_s.at[k - 1], zs_r.at[k - 1], (z_of[k], r, t))
        c.start()
        zc.append(c)
    for k in stages[0]:
        spread(k)
    for c in zc:
        c.wait_recv()
    proj = z_ref[0].astype(F32)
    for k in range(1, nz):
        proj = proj + z_ref[k].astype(F32)
    q1, q2, qr = moments(proj[:, :qc], q1_ref[...], q2_ref[...])
    v1, v2, vr = moments(proj[:, qc:], v1_ref[...], v2_ref[...])
    ratio_ref[low_rows(r), :qc] = qr.astype(BF)
    ratio_ref[low_rows(r), qc:] = vr.astype(BF)
    agc = []
    for j in range(1, nr):
        here = ratio_ref.at[low_rows(r)]
        c = remote(here, here, ag_s.at[j - 1], ag_r.at[j - 1], (z, r_of[j], t))
        c.start()
        agc.append(c)
    first_out[:, :qc] = q1
    first_out[:, qc:] = v1
    second_out[:, :qc] = q2
    second_out[:, qc:] = v2
    for k in stages[0]:
        relay(k)
    for k in stages[1]:
        spread(k)
    for k in stages[1]:
        relay(k)
    for k in stages[2]:
        spread(k)
    fx.wait_recv()
    for c in agc:
        c.wait_recv()
    step = min(256, width)

    def squares(i, acc):
        span = pl.ds(pl.multiple_of(i * step, step), step)
        a = jnp.dot(f_ref[0, span], ratio_ref[:, :qc], preferred_element_type=F32)
        b = jnp.dot(f_ref[1, span], ratio_ref[:, qc:], preferred_element_type=F32)
        a = jnp.sum(a * a, axis=0, keepdims=True)
        b = jnp.sum(b * b, axis=0, keepdims=True)
        return (acc[0] + a, acc[1] + b)

    qs, vs = lax.fori_loop(
        0,
        width // step,
        squares,
        (jnp.zeros((1, qc), F32), jnp.zeros((1, cols - qc), F32)),
    )
    qs = jnp.sum(qs, axis=1, keepdims=True)
    vs = jnp.sum(vs, axis=1, keepdims=True)
    row = lax.broadcasted_iota(jnp.int32, sq_ref.shape[1:], 0)
    sq_ref[t] = jnp.where(row == 0, qs / (width * qc * 2), vs / (width * (cols - qc) * 2))
    sx = remote(sq_ref.at[t], sq_ref.at[t], tp_s.at[2], tp_r.at[2], (z, r, other))
    sx.start()
    sx.wait_recv()
    scale_out[...] = lax.rsqrt(sq_ref[0] + sq_ref[1] + EPS_NORM)
    for k in stages[2]:
        relay(k)
    for k in range(1, nz):
        w2[k, 2].wait_recv()
        w2[k, 3].wait_recv()
    for c in f1 + w1 + f2 + rsc + zc + agc + [fx, lx, sx] + list(w2.values()):
        c.wait_send()
    w_own.wait()


def run_exchange(nz, nr, x, cq, cv, wq, wv, qf, vf, q1, q2, v1, v2):
    tokens, width = x.shape
    qc = cq.shape[1]
    cols = qc + cv.shape[1]
    rows, rank = qf.shape
    own = rank // nr
    any_spec = pl.BlockSpec(memory_space=pl.ANY)
    vmem = pl.BlockSpec(memory_space=pltpu.VMEM)
    dma = pltpu.SemaphoreType.DMA
    shape = jax.ShapeDtypeStruct
    return pl.pallas_call(
        functools.partial(exchange, nz, nr),
        out_shape=(
            shape((width, cols), BF),
            shape((2, width, rank), BF),
            shape((rank, cols), BF),
            shape((own, cols), F32),
            shape((own, cols), F32),
            shape((8, 128), F32),
        ),
        in_specs=[any_spec] * 7 + [vmem] * 4,
        out_specs=(any_spec, vmem, vmem, vmem, vmem, vmem),
        scratch_shapes=[
            pltpu.VMEM((tokens, width), BF),
            pltpu.VMEM(cq.shape, BF),
            pltpu.VMEM(cv.shape, BF),
            pltpu.VMEM((rows, cols), F32),
            pltpu.VMEM((rows, cols), BF),
            pltpu.VMEM((2, tokens, rank), BF),
            pltpu.VMEM((rank, cols), BF),
            pltpu.VMEM((nr - 1, own, cols), BF),
            pltpu.VMEM((nz, own, cols), BF),
            pltpu.VMEM((2, 8, 128), F32),
            dma((7,)),
            dma((nz - 1,)),
            dma((nz - 1,)),
            dma((nz - 1,)),
            dma((nz - 1,)),
            dma(((nz - 1) * (nr - 1),)),
            dma(((nz - 1) * (nr - 1),)),
            dma((nz - 1, 4)),
            dma((nz - 1, 4)),
            dma((nr - 1,)),
            dma((nr - 1,)),
            dma((nz - 1,)),
            dma((nz - 1,)),
            dma((nr - 1,)),
            dma((nr - 1,)),
            dma((3,)),
            dma((3,)),
        ],
        compiler_params=pltpu.CompilerParams(
            collective_id=0, has_side_effects=True, vmem_limit_bytes=48 * 1024 * 1024
        ),
    )(x, cq, cv, wq, wv, qf, vf, q1, q2, v1, v2)


def local(
    nz,
    nr,
    saved_inputs,
    query_cotangent,
    value_cotangent,
    query_weight,
    value_weight,
    query_factor,
    value_factor,
    query_first,
    query_second,
    value_first,
    value_second,
):
    qc = query_cotangent.shape[1]
    rows = query_weight.shape[0]
    weights, factors, ratio, first, second, scale = run_exchange(
        nz,
        nr,
        saved_inputs,
        query_cotangent,
        value_cotangent,
        query_weight,
        value_weight,
        query_factor,
        value_factor,
        query_first,
        query_second,
        value_first,
        value_second,
    )
    query_scale = scale[0, 0]
    value_scale = scale[1, 0]
    query_raw = jnp.dot(factors[0], ratio[:, :qc], preferred_element_type=F32)
    value_raw = jnp.dot(factors[1], ratio[:, qc:], preferred_element_type=F32)
    query_copy = (weights[:, :qc].astype(F32) - RATE * (query_raw * query_scale)).astype(BF)
    value_copy = (weights[:, qc:].astype(F32) - RATE * (value_raw * value_scale)).astype(BF)
    query_direction = query_scale * jnp.dot(
        query_factor, ratio[:, :qc], preferred_element_type=F32
    )
    value_direction = value_scale * jnp.dot(
        value_factor, ratio[:, qc:], preferred_element_type=F32
    )
    query_master = query_weight - RATE * query_direction
    value_master = value_weight - RATE * value_direction
    return (
        query_direction,
        value_direction,
        query_master,
        value_master,
        first[:, :qc],
        second[:, :qc],
        first[:, qc:],
        second[:, qc:],
        query_copy,
        value_copy,
    )


def solution(mesh):
    return jax.shard_map(
        functools.partial(local, mesh.shape["fs"], mesh.shape["rep"]),
        mesh=mesh,
        in_specs=(
            P(("fs", "rep"), None),
            P(("fs", "rep"), "tp"),
            P(("fs", "rep"), "tp"),
            P("fs", "tp"),
            P("fs", "tp"),
            P("fs", None),
            P("fs", None),
            P("rep", "tp"),
            P("rep", "tp"),
            P("rep", "tp"),
            P("rep", "tp"),
        ),
        out_specs=(
            P("fs", "tp"),
            P("fs", "tp"),
            P("fs", "tp"),
            P("fs", "tp"),
            P("rep", "tp"),
            P("rep", "tp"),
            P("rep", "tp"),
            P("rep", "tp"),
            P(None, "tp"),
            P(None, "tp"),
        ),
        check_vma=False,
    )
```

```python
import functools

import jax
import jax.numpy as jnp
from jax import lax
from jax.experimental import pallas as pl
from jax.experimental.pallas import tpu as pltpu
from jax.sharding import PartitionSpec as P

BETA_ONE = 0.8
BETA_TWO = 0.9
EPS_RATIO = 1e-08
EPS_NORM = 1e-06
RATE = 0.02
BF = jnp.bfloat16
F32 = jnp.float32


def moments(projected, first, second):
    first_new = BETA_ONE * first + (1.0 - BETA_ONE) * projected
    second_new = BETA_TWO * second + (1.0 - BETA_TWO) * projected * projected
    ratio = first_new / (jnp.sqrt(second_new) + EPS_RATIO)
    return (first_new, second_new, ratio)


def exchange(
    nz,
    nr,
    x_hbm,
    cq_hbm,
    cv_hbm,
    wq_hbm,
    wv_hbm,
    qf_hbm,
    vf_hbm,
    q1_hbm,
    q2_hbm,
    v1_hbm,
    v2_hbm,
    w_out,
    f_ref,
    ratio_ref,
    proj_out,
    scale_out,
    x_ref,
    cq_ref,
    cv_ref,
    wf_ref,
    wb_ref,
    low_ref,
    part_ref,
    rs_ref,
    z_ref,
    zg_ref,
    zh_ref,
    m1_ref,
    m2_ref,
    sq_ref,
    local_sem,
    f1_s,
    f1_r,
    w1_s,
    w1_r,
    f2_s,
    f2_r,
    w2_s,
    w2_r,
    rs_s,
    rs_r,
    zs_s,
    zs_r,
    zg_s,
    zg_r,
    ag_s,
    ag_r,
    tp_s,
    tp_r,
):
    z = lax.axis_index("fs")
    r = lax.axis_index("rep")
    t = lax.axis_index("tp")
    rows = qf_hbm.shape[0]
    part = rows // nr
    qc = cq_ref.shape[1]
    cols = w_out.shape[1]
    half = cols // 2
    width = w_out.shape[0]
    rank = low_ref.shape[2]
    own = rank // nr
    tokens = x_ref.shape[0]
    z_of = [lax.rem(z + k, nz) for k in range(nz)]
    z_from = [lax.rem(z + nz - k, nz) for k in range(nz)]
    r_of = [lax.rem(r + j, nr) for j in range(nr)]
    side = r + 1 - 2 * lax.rem(r, 2)
    over = lax.rem(r + 2, nr)
    corner = nr - 1 - r
    other = 1 - t

    def remote(src, dst, ss, rs, dev):
        return pltpu.make_async_remote_copy(
            src_ref=src,
            dst_ref=dst,
            send_sem=ss,
            recv_sem=rs,
            device_id=dev,
            device_id_type=pl.DeviceIdType.MESH,
        )

    def slab(zz, rr):
        return pl.ds(pl.multiple_of(zz * rows + rr * part, part), part)

    def fac_copy(src):
        return pltpu.make_async_copy(
            src,
            f_ref.at[t, pl.ds(pl.multiple_of(z * rows, rows), rows)],
            local_sem.at[0],
        )

    @pl.when(t == 0)
    def _():
        fac_copy(qf_hbm).start()

    @pl.when(t == 1)
    def _():
        fac_copy(vf_hbm).start()

    wq_in = pltpu.make_async_copy(wq_hbm, wf_ref.at[:, pl.ds(0, qc)], local_sem.at[1])
    wv_in = pltpu.make_async_copy(wv_hbm, wf_ref.at[:, pl.ds(qc, cols - qc)], local_sem.at[2])
    x_in = pltpu.make_async_copy(x_hbm, x_ref, local_sem.at[3])
    cq_in = pltpu.make_async_copy(cq_hbm, cq_ref, local_sem.at[4])
    cv_in = pltpu.make_async_copy(cv_hbm, cv_ref, local_sem.at[5])
    left, right = pl.ds(0, qc), pl.ds(qc, cols - qc)
    mom = [
        pltpu.make_async_copy(src, dst.at[:, at], local_sem.at[7 + n])
        for n, (src, dst, at) in enumerate(
            (
                (q1_hbm, m1_ref, left),
                (v1_hbm, m1_ref, right),
                (q2_hbm, m2_ref, left),
                (v2_hbm, m2_ref, right),
            )
        )
    ]
    for c in [wq_in, wv_in, x_in, cq_in, cv_in] + mom:
        c.start()

    barrier = pltpu.get_barrier_semaphore()
    peers = [(z_of[k], r, t) for k in range(1, nz)]
    peers += [(z, r_of[j], t) for j in range(1, nr)]
    peers += [(z, r, other)]
    for dev in peers:
        pl.semaphore_signal(
            barrier, inc=1, device_id=dev, device_id_type=pl.DeviceIdType.MESH
        )
    pl.semaphore_wait(barrier, len(peers))

    fac_copy(qf_hbm).wait()
    sends = []
    f1 = []
    for k in range(1, nz):
        here = f_ref.at[t, slab(z, r)]
        c = remote(here, here, f1_s.at[k - 1], f1_r.at[k - 1], (z_of[k], r, t))
        c.start()
        f1.append(c)
    wq_in.wait()
    wv_in.wait()
    wb_ref[...] = wf_ref[...].astype(BF)
    w1 = []
    for k in range(1, nz):
        c = remote(
            wb_ref.at[pl.ds(pl.multiple_of(r * part, part), part)],
            w_out.at[slab(z, r)],
            w1_s.at[k - 1],
            w1_r.at[k - 1],
            (z_of[k], r, t),
        )
        c.start()
        w1.append(c)
    w_own = pltpu.make_async_copy(
        wb_ref, w_out.at[pl.ds(pl.multiple_of(z * rows, rows), rows)], local_sem.at[6]
    )
    w_own.start()

    f2 = []
    for k in range(1, nz):
        f1[k - 1].wait_recv()
        there = f_ref.at[t, slab(z_from[k], r)]
        for j in range(1, nr):
            n = (k - 1) * (nr - 1) + j - 1
            c = remote(there, there, f2_s.at[n], f2_r.at[n], (z, r_of[j], t))
            c.start()
            f2.append(c)
    for c in f2:
        c.wait_recv()
    w2 = {}

    def spread(k):
        w1[k - 1].wait_recv()
        there = w_out.at[slab(z_from[k], r)]
        for n, dev in ((0, side), (1, over)):
            c = remote(there, there, w2_s.at[k - 1, n], w2_r.at[k - 1, n], (z, dev, t))
            c.start()
            w2[k, n] = c

    def relay(k):
        for n, src, dev, at in ((0, side, over, 0), (1, over, side, half)):
            w2[k, n].wait_recv()
            there = w_out.at[slab(z_from[k], src), pl.ds(at, half)]
            c = remote(
                there, there, w2_s.at[k - 1, 2 + n], w2_r.at[k - 1, 2 + n], (z, dev, t)
            )
            c.start()
            w2[k, 2 + n] = c

    stages = [[], [], []]
    for k in range(1, nz):
        stages[min(k - 1, 2)].append(k)
    for k in stages[0]:
        spread(k)
    fx = remote(f_ref.at[t], f_ref.at[t], tp_s.at[0], tp_r.at[0], (z, r, other))
    fx.start()
    x_in.wait()
    tile = tokens // 3

    @pl.loop(0, 3)
    def _(i):
        span = pl.ds(pl.multiple_of(i * tile, tile), tile)
        low_ref[t, span] = jnp.dot(
            x_ref[span, :], f_ref[t], preferred_element_type=F32
        ).astype(BF)

    lx = remote(low_ref.at[t], low_ref.at[t], tp_s.at[1], tp_r.at[1], (z, r, other))
    lx.start()
    cq_in.wait()
    cv_in.wait()
    lx.wait_recv()
    dims = (((0,), (0,)), ((), ()))
    part_ref[:, :qc] = lax.dot_general(
        low_ref[0], cq_ref[...], dims, preferred_element_type=F32
    ).astype(BF)
    part_ref[:, qc:] = lax.dot_general(
        low_ref[1], cv_ref[...], dims, preferred_element_type=F32
    ).astype(BF)

    def low_rows(rr):
        return pl.ds(pl.multiple_of(rr * own, own), own)

    rsc = []
    for j in range(1, nr):
        c = remote(
            part_ref.at[low_rows(r_of[j])],
            rs_ref.at[j - 1],
            rs_s.at[j - 1],
            rs_r.at[j - 1],
            (z, r_of[j], t),
        )
        c.start()
        rsc.append(c)

    for k in stages[0]:
        relay(k)
    for c in rsc:
        c.wait_recv()
    total = part_ref[low_rows(r), :].astype(F32)
    for j in range(1, nr):
        total = total + rs_ref[j - 1].astype(F32)
    share = own // nz
    scatter = share % 16 == 0
    zc = []
    if scatter:
        zg_ref[...] = total.astype(BF)
    else:
        z_ref[z] = total.astype(BF)

    def z_rows(zz):
        return pl.ds(pl.multiple_of(zz * share, share), share)

    for k in range(1, nz):
        src = zg_ref.at[z_rows(z_of[k])] if scatter else z_ref.at[z]
        c = remote(src, z_ref.at[z], zs_s.at[k - 1], zs_r.at[k - 1], (z_of[k], r, t))
        c.start()
        zc.append(c)
    if scatter:
        z_ref[z] = zg_ref[z_rows(z), :]
    for k in stages[1]:
        spread(k)
    for c in zc:
        c.wait_recv()
    proj = z_ref[0].astype(F32)
    for k in range(1, nz):
        proj = proj + z_ref[k].astype(F32)
    gc = []
    if scatter:
        for c in zc:
            c.wait_send()
        zh = zh_ref
        zh[z_rows(z), :] = proj.astype(BF)
        for k in range(1, nz):
            here = zh.at[z_rows(z)]
            c = remote(here, here, zg_s.at[k - 1], zg_r.at[k - 1], (z_of[k], r, t))
            c.start()
            gc.append(c)
    for k in stages[1]:
        relay(k)
    for k in stages[2]:
        spread(k)
    for c in mom:
        c.wait()
    if scatter:
        for c in gc:
            c.wait_recv()
        proj = zh[...].astype(F32)
    proj_out[...] = proj
    _, _, ratio = moments(proj, m1_ref[...], m2_ref[...])
    ratio_ref[low_rows(r), :] = ratio.astype(BF)
    agc = []
    for j in range(1, nr):
        here = ratio_ref.at[low_rows(r)]
        c = remote(here, here, ag_s.at[j - 1], ag_r.at[j - 1], (z, r_of[j], t))
        c.start()
        agc.append(c)
    for k in stages[2]:
        relay(k)
    fx.wait_recv()
    for c in agc:
        c.wait_recv()
    step = min(256, width)

    def squares(i, acc):
        span = pl.ds(pl.multiple_of(i * step, step), step)
        a = jnp.dot(f_ref[0, span], ratio_ref[:, :qc], preferred_element_type=F32)
        b = jnp.dot(f_ref[1, span], ratio_ref[:, qc:], preferred_element_type=F32)
        a = jnp.sum(a * a, axis=0, keepdims=True)
        b = jnp.sum(b * b, axis=0, keepdims=True)
        return (acc[0] + a, acc[1] + b)

    qs, vs = lax.fori_loop(
        0,
        width // step,
        squares,
        (jnp.zeros((1, qc), F32), jnp.zeros((1, cols - qc), F32)),
    )
    qs = jnp.sum(qs, axis=1, keepdims=True)
    vs = jnp.sum(vs, axis=1, keepdims=True)
    row = lax.broadcasted_iota(jnp.int32, sq_ref.shape[1:], 0)
    sq_ref[t] = jnp.where(row == 0, qs / (width * qc * 2), vs / (width * (cols - qc) * 2))
    sx = remote(sq_ref.at[t], sq_ref.at[t], tp_s.at[2], tp_r.at[2], (z, r, other))
    sx.start()
    sx.wait_recv()
    scale_out[...] = lax.rsqrt(sq_ref[0] + sq_ref[1] + EPS_NORM)
    for k in range(1, nz):
        w2[k, 2].wait_recv()
        w2[k, 3].wait_recv()
    for c in f1 + w1 + f2 + rsc + ([] if scatter else zc) + gc + agc + [fx, lx, sx] + list(w2.values()):
        c.wait_send()
    w_own.wait()


def run_exchange(nz, nr, x, cq, cv, wq, wv, qf, vf, q1, q2, v1, v2):
    tokens, width = x.shape
    qc = cq.shape[1]
    cols = qc + cv.shape[1]
    rows, rank = qf.shape
    own = rank // nr
    share = own // nz if (own // nz) % 16 == 0 else own
    any_spec = pl.BlockSpec(memory_space=pltpu.HBM)
    vmem = pl.BlockSpec(memory_space=pltpu.VMEM)
    dma = pltpu.SemaphoreType.DMA
    shape = jax.ShapeDtypeStruct
    return pl.pallas_call(
        functools.partial(exchange, nz, nr),
        out_shape=(
            shape((width, cols), BF),
            shape((2, width, rank), BF),
            shape((rank, cols), BF),
            shape((own, cols), F32),
            shape((8, 128), F32),
        ),
        in_specs=[any_spec] * 11,
        out_specs=(any_spec, vmem, vmem, vmem, vmem),
        scratch_shapes=[
            pltpu.VMEM((tokens, width), BF),
            pltpu.VMEM(cq.shape, BF),
            pltpu.VMEM(cv.shape, BF),
            pltpu.VMEM((rows, cols), F32),
            pltpu.VMEM((rows, cols), BF),
            pltpu.VMEM((2, tokens, rank), BF),
            pltpu.VMEM((rank, cols), BF),
            pltpu.VMEM((nr - 1, own, cols), BF),
            pltpu.VMEM((nz, share, cols), BF),
            pltpu.VMEM((own, cols), BF),
            pltpu.VMEM((own, cols), BF),
            pltpu.VMEM((own, cols), F32),
            pltpu.VMEM((own, cols), F32),
            pltpu.VMEM((2, 8, 128), F32),
            dma((11,)),
            dma((nz - 1,)),
            dma((nz - 1,)),
            dma((nz - 1,)),
            dma((nz - 1,)),
            dma(((nz - 1) * (nr - 1),)),
            dma(((nz - 1) * (nr - 1),)),
            dma((nz - 1, 4)),
            dma((nz - 1, 4)),
            dma((nr - 1,)),
            dma((nr - 1,)),
            dma((nz - 1,)),
            dma((nz - 1,)),
            dma((nz - 1,)),
            dma((nz - 1,)),
            dma((nr - 1,)),
            dma((nr - 1,)),
            dma((3,)),
            dma((3,)),
        ],
        compiler_params=pltpu.CompilerParams(
            collective_id=0, has_side_effects=True, vmem_limit_bytes=60 * 1024 * 1024
        ),
    )(x, cq, cv, wq, wv, qf, vf, q1, q2, v1, v2)


def finish(
    f_ref,
    ratio_ref,
    scale_ref,
    w_ref,
    wq_ref,
    wv_ref,
    qf_ref,
    vf_ref,
    proj_ref,
    q1_ref,
    q2_ref,
    v1_ref,
    v2_ref,
    qd_out,
    vd_out,
    qm_out,
    vm_out,
    q1_out,
    q2_out,
    v1_out,
    v2_out,
    qcopy_out,
    vcopy_out,
):
    qc = wq_ref.shape[1]
    sets = (
        (0, pl.ds(0, qc), wq_ref, qf_ref, q1_ref, q2_ref, qd_out, qm_out, q1_out, q2_out, qcopy_out),
        (
            1,
            pl.ds(qc, wv_ref.shape[1]),
            wv_ref,
            vf_ref,
            v1_ref,
            v2_ref,
            vd_out,
            vm_out,
            v1_out,
            v2_out,
            vcopy_out,
        ),
    )
    for n, at, w, f, m1, m2, d_out, m_out, m1_out, m2_out, c_out in sets:
        scale = scale_ref[n : n + 1, 0:1]
        ratio = ratio_ref[:, at]
        raw = jnp.dot(f_ref[n], ratio, preferred_element_type=F32)
        c_out[...] = (w_ref[:, at].astype(F32) - RATE * (raw * scale)).astype(BF)
        d = jnp.dot(f[...], ratio, preferred_element_type=F32) * scale
        d_out[...] = d
        m_out[...] = w[...] - RATE * d
        m1_out[...], m2_out[...], _ = moments(proj_ref[:, at], m1[...], m2[...])


def run_finish(factors, ratio, scale, weights, wq, wv, qf, vf, proj, q1, q2, v1, v2):
    rows, qc = wq.shape
    vc = wv.shape[1]
    width, cols = weights.shape
    rank, own = qf.shape[1], q1.shape[0]
    steps = 8 if rows % 128 == 0 else 4

    def tall(n, c):
        return pl.BlockSpec((n // steps, c), lambda i: (i, 0))

    def whole(a):
        return pl.BlockSpec(a.shape, lambda i: (0,) * a.ndim)

    shape = jax.ShapeDtypeStruct
    return pl.pallas_call(
        finish,
        grid=(steps,),
        in_specs=[
            pl.BlockSpec((2, width // steps, rank), lambda i: (0, i, 0)),
            whole(ratio),
            whole(scale),
            tall(width, cols),
            tall(rows, qc),
            tall(rows, vc),
            tall(rows, rank),
            tall(rows, rank),
            tall(own, cols),
            tall(own, qc),
            tall(own, qc),
            tall(own, vc),
            tall(own, vc),
        ],
        out_specs=[
            tall(rows, qc),
            tall(rows, vc),
            tall(rows, qc),
            tall(rows, vc),
            tall(own, qc),
            tall(own, qc),
            tall(own, vc),
            tall(own, vc),
            tall(width, qc),
            tall(width, vc),
        ],
        out_shape=[
            shape((rows, qc), F32),
            shape((rows, vc), F32),
            shape((rows, qc), F32),
            shape((rows, vc), F32),
            shape((own, qc), F32),
            shape((own, qc), F32),
            shape((own, vc), F32),
            shape((own, vc), F32),
            shape((width, qc), BF),
            shape((width, vc), BF),
        ],
        compiler_params=pltpu.CompilerParams(vmem_limit_bytes=60 * 1024 * 1024),
    )(factors, ratio, scale, weights, wq, wv, qf, vf, proj, q1, q2, v1, v2)


def local(nz, nr, *args):
    _, _, _, wq, wv, qf, vf, q1, q2, v1, v2 = args
    weights, factors, ratio, proj, scale = run_exchange(nz, nr, *args)
    return tuple(
        run_finish(factors, ratio, scale, weights, wq, wv, qf, vf, proj, q1, q2, v1, v2)
    )


def solution(mesh):
    return jax.shard_map(
        functools.partial(local, mesh.shape["fs"], mesh.shape["rep"]),
        mesh=mesh,
        in_specs=(
            P(("fs", "rep"), None),
            P(("fs", "rep"), "tp"),
            P(("fs", "rep"), "tp"),
            P("fs", "tp"),
            P("fs", "tp"),
            P("fs", None),
            P("fs", None),
            P("rep", "tp"),
            P("rep", "tp"),
            P("rep", "tp"),
            P("rep", "tp"),
        ),
        out_specs=(
            P("fs", "tp"),
            P("fs", "tp"),
            P("fs", "tp"),
            P("fs", "tp"),
            P("rep", "tp"),
            P("rep", "tp"),
            P("rep", "tp"),
            P("rep", "tp"),
            P(None, "tp"),
            P(None, "tp"),
        ),
        check_vma=False,
    )
```
